32 devices in a mesh: sp: 16 (over z, y, x), tp: 2 (over core).
Axes of the slice: x: 2, y: 2, z: 4, core: 2. Of those that a mesh axis runs over, the one named last changes fastest.
Arguments:
- resid: bfloat16 [2048, 2048], P('sp', 'tp'), may hold values from -6 to 6
- qa_nope: bfloat16 [2048, 1024], P('sp', 'tp'), may hold values from -6 to 6
- qb_nope: bfloat16 [2048, 1024], P('sp', 'tp'), may hold values from -6 to 6
- qa_rope: bfloat16 [2048, 512], P('sp', 'tp'), may hold values from -360 to 360
- qb_rope: bfloat16 [2048, 256], P('sp', 'tp'), may hold values from -360 to 360
- latent: bfloat16 [2048, 256], P('sp'), may hold values from -6 to 6
- key_rope: bfloat16 [2048, 32], P('sp'), may hold values from -4 to 4
- lat_gain: float32 [256], replicated, may hold values from 0.1 to 1.9
- wa_key: bfloat16 [256, 1024], P(None, 'tp'), may hold values from -0.375 to 0.375
- wa_val: bfloat16 [256, 1024], P(None, 'tp'), may hold values from -0.75 to 0.75
- wb_key: bfloat16 [256, 1024], P(None, 'tp'), may hold values from -0.375 to 0.375
- wb_val: bfloat16 [256, 1024], P(None, 'tp'), may hold values from -0.75 to 0.75
- gain_a: float32 [1024], P('tp'), may hold values from 0.1 to 1.9
- gain_b: float32 [1024], P('tp'), may hold values from 0.1 to 1.9
- wa_out: bfloat16 [1024, 2048], P('tp'), may hold values from -0.125 to 0.125
- wb_out: bfloat16 [1024, 2048], P('tp'), may hold values from -0.125 to 0.125
- norm1_gain: float32 [2048], replicated, may hold values from 0.1 to 1.9
- ffn_gate: bfloat16 [2048, 5632], P('sp', 'tp'), may hold values from -0.125 to 0.125
- ffn_val: bfloat16 [2048, 5632], P('sp', 'tp'), may hold values from -0.125 to 0.125
- conv_gate: float32 [3, 5632], P(None, 'tp'), may hold values from -3 to 3
- conv_val: float32 [3, 5632], P(None, 'tp'), may hold values from -3 to 3
- ffn_down: bfloat16 [5632, 2048], P('tp'), may hold values from -0.078125 to 0.078125
- norm2_gain: float32 [2048], P('tp'), may hold values from 0.1 to 1.9
Outputs:
- layer_out: bfloat16 [2048, 2048], P('sp', 'tp')
The draws below stay inside these ranges and needn't reach their ends.
All inputs are finite; a program needn't handle non-finite values.
Results may differ from the reference program's by a relative error of at most 0.017.
Values may be sent and summed in bfloat16 or wider, within the bound.
No kernel may reach another device: no remote copies, remote signals or barrier semaphores. Data moves between devices by JAX's collectives and lax.ppermute only.
A program may use at most 128 MiB of HBM per device.

```python
import math
import jax
import jax.numpy as jnp
from jax import lax

D = 2048
HA = 16
DA = 64
HB = 8
DB = 128
DR = 32
LAT = 256
FF = 5632
KC = 3
TOKENS = 2048


def drawn(key):
    base = jnp.clip(jax.random.normal(jax.random.fold_in(key, 101), (TOKENS, DR), jnp.float32), -4.0, 4.0)
    return base


def draw_key_rope(key, part):
    base = drawn(key)
    return base.astype(jnp.bfloat16)


def draw_qa_rope(key, part):
    noise = jnp.clip(jax.random.normal(jax.random.fold_in(key, 104), (TOKENS, HA * DR), jnp.float32), -6.0, 6.0)
    return noise.astype(jnp.bfloat16)


def draw_qb_rope(key, part):
    noise = jnp.clip(jax.random.normal(jax.random.fold_in(key, 105), (TOKENS, HB * DR), jnp.float32), -6.0, 6.0)
    return noise.astype(jnp.bfloat16)


def rising_value(key, heads, width):
    noise = jnp.clip(jax.random.normal(key, (LAT, heads * width), jnp.float32), -6.0, 6.0) * LAT ** (-0.5)
    head_index = (jnp.arange(heads * width) // width).astype(jnp.float32)
    factor = 0.5 * 4.0 ** (head_index / (heads - 1))
    return (noise * factor[None, :]).astype(jnp.bfloat16)


def draw_wa_val(key, part):
    return rising_value(jax.random.fold_in(key, 201), HA, DA)


def draw_wb_val(key, part):
    return rising_value(jax.random.fold_in(key, 202), HB, DB)


def levels(stream_key, extent, shards, least, top_value):
    loudness = 1.0
    for dim, shards_of in shards:
        draws = jax.random.uniform(jax.random.fold_in(jax.random.fold_in(stream_key, 6), dim), (shards_of,), jnp.float32, least / len(shards), top_value / len(shards))
        loudness = loudness * jnp.repeat(jnp.exp(draws), extent[dim] // shards_of).reshape((-1,) + (1,) * (len(extent) - 1 - dim))
    return loudness


def gaussian(key, shape, scale, bound, cuts=(), kind=jnp.bfloat16):
    result = scale * jax.random.normal(key, shape, jnp.float32)
    if cuts:
        result = result * levels(key, shape, cuts, -0.22, 0.18)
    return jnp.clip(result, -bound, bound).astype(kind)


def setup_inputs(seed: int = 0) -> dict:
    key_list = jax.random.split(jax.random.key(seed), 24)
    resid = gaussian(key_list[0], (TOKENS, D), 1.0, 6.0, ((0, 16), (1, 2)))
    qa_nope = gaussian(key_list[1], (TOKENS, HA * DA), 1.0, 6.0, ((0, 16), (1, 2)))
    qb_nope = gaussian(key_list[2], (TOKENS, HB * DB), 1.0, 6.0, ((0, 16), (1, 2)))
    qa_rope = draw_qa_rope(jax.random.fold_in(key_list[23], 71), 0)
    qb_rope = draw_qb_rope(jax.random.fold_in(key_list[23], 71), 0)
    latent = gaussian(key_list[5], (TOKENS, LAT), 1.0, 6.0, ((0, 16),))
    key_rope = draw_key_rope(jax.random.fold_in(key_list[23], 71), 0)
    lat_gain = jnp.clip(1.0 + 0.18 * jax.random.normal(key_list[7], (LAT,), jnp.float32), 0.1, 1.9)
    wa_key = gaussian(key_list[8], (LAT, HA * DA), LAT ** -0.5, 0.375, ((1, 2),))
    wa_val = draw_wa_val(jax.random.fold_in(key_list[23], 71), 0)
    wb_key = gaussian(key_list[10], (LAT, HB * DB), LAT ** -0.5, 0.375, ((1, 2),))
    wb_val = draw_wb_val(jax.random.fold_in(key_list[23], 71), 0)
    gain_a = jnp.clip(1.0 + 0.18 * jax.random.normal(key_list[12], (HA * DA,), jnp.float32), 0.1, 1.9)
    gain_b = jnp.clip(1.0 + 0.18 * jax.random.normal(key_list[13], (HB * DB,), jnp.float32), 0.1, 1.9)
    wa_out = gaussian(key_list[14], (HA * DA, D), (HA * DA + HB * DB) ** -0.5, 0.125, ((0, 2),))
    wb_out = gaussian(key_list[15], (HB * DB, D), (HA * DA + HB * DB) ** -0.5, 0.125, ((0, 2),))
    norm1_gain = jnp.clip(1.0 + 0.18 * jax.random.normal(key_list[16], (D,), jnp.float32), 0.1, 1.9)
    ffn_gate = gaussian(key_list[17], (D, FF), D ** -0.5, 0.125, ((0, 16), (1, 2)))
    ffn_val = gaussian(key_list[18], (D, FF), D ** -0.5, 0.125, ((0, 16), (1, 2)))
    conv_gate = gaussian(key_list[19], (KC, FF), 0.577, 3.0, ((1, 2),), jnp.float32)
    conv_val = gaussian(key_list[20], (KC, FF), 0.577, 3.0, ((1, 2),), jnp.float32)
    ffn_down = gaussian(key_list[21], (FF, D), FF ** -0.5, 0.078125, ((0, 2),))
    norm2_gain = jnp.clip(1.0 + 0.18 * jax.random.normal(key_list[22], (D,), jnp.float32), 0.1, 1.9)
    return dict(resid=resid, qa_nope=qa_nope, qb_nope=qb_nope, qa_rope=qa_rope, qb_rope=qb_rope, latent=latent, key_rope=key_rope, lat_gain=lat_gain, wa_key=wa_key, wa_val=wa_val, wb_key=wb_key, wb_val=wb_val, gain_a=gain_a, gain_b=gain_b, wa_out=wa_out, wb_out=wb_out, norm1_gain=norm1_gain, ffn_gate=ffn_gate, ffn_val=ffn_val, conv_gate=conv_gate, conv_val=conv_val, ffn_down=ffn_down, norm2_gain=norm2_gain)


THETA = 10000.0
EPS_RMS = 1e-06
EPS_NORM = 1e-05
ALPHA = 2.0 ** 0.25

def stored(values):
    return lax.optimization_barrier(values.astype(jnp.bfloat16))

def rotary(values, positions):
    half = values.shape[-1] // 2
    freq = THETA ** (-jnp.arange(half, dtype=jnp.float32) * 2.0 / values.shape[-1])
    angle = positions.astype(jnp.float32)[:, None] * freq[None, :]
    if values.ndim == 3:
        angle = angle[:, None, :]
    cosine = jnp.cos(angle)
    sine = jnp.sin(angle)
    first = values[..., :half]
    second = values[..., half:]
    return jnp.concatenate([first * cosine - second * sine, second * cosine + first * sine], axis=-1)

def rms_scale(values, gain):
    wide = values.astype(jnp.float32)
    return wide * lax.rsqrt(lax.optimization_barrier(jnp.mean(wide * wide, axis=-1, keepdims=True)) + EPS_RMS) * gain.astype(jnp.float32)

def layer_norm(values, gain):
    center = lax.optimization_barrier(jnp.mean(values, axis=-1, keepdims=True))
    shifted = values - center
    spread = lax.optimization_barrier(jnp.mean(shifted * shifted, axis=-1, keepdims=True))
    return shifted * lax.rsqrt(spread + EPS_NORM) * gain.astype(jnp.float32)

def attend(query, q_rot, keys, k_rot, vals):
    total_rows, heads, width = query.shape
    scale = (width + k_rot.shape[-1]) ** (-0.5)
    block = math.gcd(512, total_rows)
    key_pos = jnp.arange(total_rows)
    keys_wide = keys.astype(jnp.float32)
    rot_wide = k_rot.astype(jnp.float32)
    vals_wide = vals.astype(jnp.float32)

    def one_block(index):
        start = index * block
        q_part = lax.dynamic_slice_in_dim(query, start, block, 0).astype(jnp.float32)
        r_part = lax.dynamic_slice_in_dim(q_rot, start, block, 0).astype(jnp.float32)
        scores = jnp.einsum('qhd,khd->hqk', q_part, keys_wide) + jnp.einsum('qhr,kr->hqk', r_part, rot_wide)
        scores = scores * scale
        q_pos = start + jnp.arange(block)
        allowed = key_pos[None, :] <= q_pos[:, None]
        scores = jnp.where(allowed[None], scores, -jnp.inf)
        top = lax.optimization_barrier(jnp.max(scores, axis=-1, keepdims=True))
        weights = jnp.exp(scores - top)
        total = lax.optimization_barrier(jnp.sum(weights, axis=-1))
        rounded = stored(weights).astype(jnp.float32)
        mixed = jnp.einsum('hqk,khd->qhd', rounded, vals_wide)
        return mixed / jnp.transpose(total)[:, :, None]
    out = lax.map(one_block, jnp.arange(total_rows // block)).reshape(total_rows, heads * width)
    return out

def causal_conv(values, taps):
    count = values.shape[0]
    padded = jnp.pad(values.astype(jnp.float32), ((KC - 1, 0), (0, 0)))
    total = jnp.zeros(values.shape, jnp.float32)
    for tap in range(KC):
        total = total + taps[tap].astype(jnp.float32) * padded[tap:tap + count]
    return total

def reference(resid, qa_nope, qb_nope, qa_rope, qb_rope, latent, key_rope, lat_gain, wa_key, wa_val, wb_key, wb_val, gain_a, gain_b, wa_out, wb_out, norm1_gain, ffn_gate, ffn_val, conv_gate, conv_val, ffn_down, norm2_gain):
    positions = jnp.arange(TOKENS)
    lat_n = stored(rms_scale(latent, lat_gain))
    k_rot = stored(rotary(key_rope.astype(jnp.float32), positions))

    def group(q_nope, q_rope, w_key, w_val, width):
        heads = q_nope.shape[1] // width
        q_rot = stored(rotary(q_rope.astype(jnp.float32).reshape(TOKENS, heads, DR), positions))
        keys = stored(jnp.dot(lat_n, w_key, preferred_element_type=jnp.float32)).reshape(TOKENS, heads, width)
        vals = stored(jnp.dot(lat_n, w_val, preferred_element_type=jnp.float32)).reshape(TOKENS, heads, width)
        return attend(q_nope.reshape(TOKENS, heads, width), q_rot, keys, k_rot, vals)
    raw_a = group(qa_nope, qa_rope, wa_key, wa_val, DA)
    raw_b = group(qb_nope, qb_rope, wb_key, wb_val, DB)
    energy = lax.optimization_barrier(jnp.sum(raw_a * raw_a, axis=-1)) + lax.optimization_barrier(jnp.sum(raw_b * raw_b, axis=-1))
    factor = lax.rsqrt(energy / (HA * DA + HB * DB) + EPS_RMS)[:, None]
    part_a = stored(raw_a * factor * gain_a.astype(jnp.float32))
    part_b = stored(raw_b * factor * gain_b.astype(jnp.float32))
    mix = jnp.dot(part_a, wa_out, preferred_element_type=jnp.float32) + jnp.dot(part_b, wb_out, preferred_element_type=jnp.float32)
    first = stored(layer_norm(ALPHA * resid.astype(jnp.float32) + mix, norm1_gain))
    gate_up = stored(jnp.dot(first, ffn_gate, preferred_element_type=jnp.float32))
    val_up = stored(jnp.dot(first, ffn_val, preferred_element_type=jnp.float32))
    gate_c = causal_conv(gate_up, conv_gate)
    val_c = causal_conv(val_up, conv_val)
    hidden = stored(jax.nn.silu(gate_c) * val_c)
    down = jnp.dot(hidden, ffn_down, preferred_element_type=jnp.float32)
    return layer_norm(ALPHA * first.astype(jnp.float32) + down, norm2_gain).astype(jnp.bfloat16)
```

```python
import jax
import jax.numpy as jnp
from jax import lax
from jax.sharding import PartitionSpec as P

D = 2048
HA = 16
DA = 64
HB = 8
DB = 128
DR = 32
KC = 3


THETA = 10000.0
EPS_RMS = 1e-06
EPS_NORM = 1e-05
ALPHA = 2.0**0.25


def passed_along(value, axis, steps):
    count = lax.axis_size(axis)
    leading, last = (max(0, -steps), min(count, count - steps))
    return lax.ppermute(value, axis, [(source, source + steps) for source in range(leading, last)])


def rotary(values, positions):
    half = values.shape[-1] // 2
    freq = THETA ** (-jnp.arange(half, dtype=jnp.float32) * 2.0 / values.shape[-1])
    angle = positions.astype(jnp.float32)[:, None] * freq[None, :]
    if values.ndim == 3:
        angle = angle[:, None, :]
    cosine = jnp.cos(angle)
    sine = jnp.sin(angle)
    first = values[..., :half]
    second = values[..., half:]
    return jnp.concatenate(
        [first * cosine - second * sine, second * cosine + first * sine], axis=-1
    )


def rms_scale(values, gain):
    wide = values.astype(jnp.float32)
    return wide * lax.rsqrt(jnp.mean(wide * wide, axis=-1, keepdims=True) + EPS_RMS) * gain


def row_norm(values, gain):
    center = jnp.mean(values, axis=1, keepdims=True)
    shifted = values - center
    spread = jnp.mean(shifted * shifted, axis=1, keepdims=True)
    return shifted * lax.rsqrt(spread + EPS_NORM) * gain


def causal_taps(extended, taps, count):
    total = jnp.zeros(extended.shape[:1] + (count,) + extended.shape[2:], jnp.float32)
    for tap in range(KC):
        total = total + taps[tap] * extended[:, tap : tap + count].astype(jnp.float32)
    return total


def xor_swap(value, axis, mask):
    count = lax.axis_size(axis)
    return lax.ppermute(value, axis, [(source, source ^ mask) for source in range(count)])


def natural_order(items, index):
    bit = 1
    while bit < len(items):
        flip = (index & bit) != 0
        items = [jnp.where(flip, items[k ^ bit], items[k]) for k in range(len(items))]
        bit *= 2
    return items


def peer_sum(value, axis):
    if lax.axis_size(axis) == 2:
        return value + xor_swap(value, axis, 1)
    return lax.psum(value, axis)


def peer_blocks(value, axis):
    if lax.axis_size(axis) == 2:
        return jnp.stack(natural_order([value, xor_swap(value, axis, 1)], lax.axis_index(axis)))
    return lax.all_gather(value, axis, axis=0)


def doubled(value, stride, place, low_first, lead):
    bits = [1 << b for b in range(stride.bit_length() - 1)]
    if not low_first:
        bits = bits[::-1]
    spot = lead
    for bit in bits:
        other = xor_swap(value, "sp", bit)
        flip = (place & bit) != 0
        value = jnp.stack(
            [jnp.where(flip, other, value), jnp.where(flip, value, other)], axis=spot
        )
        if not low_first:
            spot += 1
    return value


def shards(
    resid,
    qa_nope,
    qb_nope,
    qa_rope,
    qb_rope,
    latent,
    key_rope,
    lat_gain,
    wa_key,
    wa_val,
    wb_key,
    wb_val,
    gain_a,
    gain_b,
    wa_out,
    wb_out,
    norm1_gain,
    ffn_gate,
    ffn_val,
    conv_gate,
    conv_val,
    ffn_down,
    norm2_gain,
):
    tok_rows = resid.shape[0]
    here = lax.axis_index("sp")
    core = lax.axis_index("tp")
    n_sp = lax.axis_size("sp")
    n_tp = lax.axis_size("tp")
    group = 4
    stride = n_sp // group
    member = here // stride
    place = here % stride
    positions = here * tok_rows + jnp.arange(tok_rows)
    heads_a = qa_nope.shape[1] // DA
    heads_b = qb_nope.shape[1] // DB
    width = ffn_gate.shape[1] // group

    share = tok_rows // n_tp
    share_pos = here * tok_rows + core * share + jnp.arange(share)
    lat_part = lax.dynamic_slice_in_dim(latent, core * share, share, 0)
    key_part = lax.dynamic_slice_in_dim(key_rope, core * share, share, 0)
    packed = jnp.concatenate(
        [
            rms_scale(lat_part, lat_gain).astype(jnp.bfloat16),
            rotary(key_part.astype(jnp.float32), share_pos).astype(jnp.bfloat16),
        ],
        axis=1,
    )
    gathered = jnp.stack(
        [packed] + [xor_swap(packed, "sp", k * stride) for k in range(1, group)]
    )
    block_of = [here ^ (k * stride) for k in range(group)]
    block_of = jnp.stack(block_of)
    bit = 1
    while bit < stride:
        gathered = jnp.concatenate([gathered, xor_swap(gathered, "sp", bit)])
        block_of = jnp.concatenate([block_of, block_of ^ bit])
        bit *= 2
    gathered = peer_blocks(gathered, "tp")
    total_keys = n_sp * tok_rows
    key_pos = (
        block_of[None, :, None] * tok_rows
        + jnp.arange(n_tp)[:, None, None] * share
        + jnp.arange(share)[None, None, :]
    ).reshape(total_keys)
    gathered = gathered.reshape(total_keys, -1)
    lat_n = gathered[:, : latent.shape[1]]
    k_rot = gathered[:, latent.shape[1] :]

    def column_block(weight, index):
        return lax.dynamic_slice_in_dim(weight, index * width, width, 1)

    def own_columns(weight, low_first):
        parts = [column_block(weight, member)] + [
            xor_swap(column_block(weight, member ^ k), "sp", k * stride) for k in range(1, group)
        ]
        parts = jnp.stack(natural_order(parts, member))
        full = doubled(parts, stride, place, low_first, 1)
        return full.reshape(n_sp * weight.shape[0], width)

    w_gate = own_columns(ffn_gate, True)
    w_val = own_columns(ffn_val, False)
    resid_full = peer_blocks(resid, "tp")

    rot_a = rotary(qa_rope.astype(jnp.float32).reshape(tok_rows, heads_a, DR), positions).astype(
        jnp.bfloat16
    )
    rot_b = rotary(qb_rope.astype(jnp.float32).reshape(tok_rows, heads_b, DR), positions).astype(
        jnp.bfloat16
    )
    query_a = qa_nope.reshape(tok_rows, heads_a, DA)
    query_b = qb_nope.reshape(tok_rows, heads_b, DB)
    allowed = key_pos[None, :] <= positions[:, None]

    def project(weight, heads, size):
        result = jnp.dot(lat_n, weight, preferred_element_type=jnp.float32).astype(jnp.bfloat16)
        return result.reshape(total_keys, heads, size)

    def attend(query, q_rot, keys, vals):
        size = query.shape[2]
        scale = (size + DR) ** (-0.5)
        scores = jnp.einsum("qhd,khd->hqk", query, keys, preferred_element_type=jnp.float32)
        scores = (
            scores + jnp.einsum("qhr,kr->hqk", q_rot, k_rot, preferred_element_type=jnp.float32)
        ) * scale
        scores = jnp.where(allowed[None], scores, -1e30)
        weights = jnp.exp(scores - jnp.max(scores, axis=-1, keepdims=True))
        total = jnp.sum(weights, axis=-1)
        mixed = jnp.einsum(
            "hqk,khd->qhd", weights.astype(jnp.bfloat16), vals, preferred_element_type=jnp.float32
        )
        mixed = mixed / jnp.transpose(total)[:, :, None]
        return mixed.reshape(tok_rows, -1)

    raw_a = attend(query_a, rot_a, project(wa_key, heads_a, DA), project(wa_val, heads_a, DA))
    raw_b = attend(query_b, rot_b, project(wb_key, heads_b, DB), project(wb_val, heads_b, DB))
    energy = jnp.sum(raw_a * raw_a, axis=1, keepdims=True) + jnp.sum(
        raw_b * raw_b, axis=1, keepdims=True
    )
    partial_value = jnp.dot(
        (raw_a * gain_a).astype(jnp.bfloat16), wa_out, preferred_element_type=jnp.float32
    ) + jnp.dot((raw_b * gain_b).astype(jnp.bfloat16), wb_out, preferred_element_type=jnp.float32)
    energy = peer_sum(energy, "tp")
    head_factor = lax.rsqrt(energy / (HA * DA + HB * DB) + EPS_RMS)
    mix = peer_sum(partial_value.astype(jnp.bfloat16), "tp").astype(jnp.float32) * head_factor
    resid_rows = jnp.concatenate([resid_full[k] for k in range(n_tp)], axis=1)
    first = row_norm(ALPHA * resid_rows.astype(jnp.float32) + mix, norm1_gain).astype(jnp.bfloat16)

    columns = resid.shape[1]
    half = lax.dynamic_slice_in_dim(first, core * columns, columns, 1)
    halves = jnp.stack(
        natural_order([half] + [xor_swap(half, "sp", k * stride) for k in range(1, group)], member)
    ).reshape(group * tok_rows, columns)
    both = peer_blocks(halves, "tp")
    first_group = jnp.concatenate([both[k] for k in range(n_tp)], axis=1)

    def up(weight):
        full = jnp.dot(first_group, weight, preferred_element_type=jnp.float32)
        return full.astype(jnp.bfloat16).reshape(group, tok_rows, width)

    def rims(value):
        ring = [
            (s, (s // stride) * stride + (s % stride + 1) % stride) for s in range(n_sp)
        ]
        rim = lax.ppermute(value[:, tok_rows - (KC - 1) :], "sp", ring)
        moved = jnp.concatenate([jnp.zeros_like(rim[:1]), rim[:-1]])
        return jnp.where(place == 0, moved, rim)

    gate_up = up(w_gate)
    rim_gate = rims(gate_up)
    val_up = up(w_val)
    rim_val = rims(val_up)
    taps_gate = column_block(conv_gate, member)
    taps_val = column_block(conv_val, member)
    gate_c = causal_taps(jnp.concatenate([rim_gate, gate_up], axis=1), taps_gate, tok_rows)
    val_c = causal_taps(jnp.concatenate([rim_val, val_up], axis=1), taps_val, tok_rows)
    hidden = (jax.nn.silu(gate_c) * val_c).astype(jnp.bfloat16)

    down_blocks = ffn_down.reshape(group, width, ffn_down.shape[1])
    down = None
    for k in range(group):
        part = lax.dynamic_index_in_dim(hidden, member ^ k, 0, keepdims=False)
        if k:
            part = xor_swap(part, "sp", k * stride)
        rows = lax.dynamic_index_in_dim(down_blocks, member ^ k, 0, keepdims=False)
        term = jnp.dot(part, rows, preferred_element_type=jnp.float32)
        down = term if down is None else down + term
    down = peer_sum(down.astype(jnp.bfloat16), "tp").astype(jnp.float32)
    pre_two = ALPHA * first.astype(jnp.float32) + down
    center = jnp.mean(pre_two, axis=1, keepdims=True)
    spread = jnp.mean((pre_two - center) * (pre_two - center), axis=1, keepdims=True)
    mine = lax.dynamic_slice_in_dim(pre_two, core * columns, columns, 1)
    return ((mine - center) * lax.rsqrt(spread + EPS_NORM) * norm2_gain).astype(jnp.bfloat16)


def solution(mesh):
    return jax.shard_map(
        shards,
        mesh=mesh,
        in_specs=(
            P("sp", "tp"),
            P("sp", "tp"),
            P("sp", "tp"),
            P("sp", "tp"),
            P("sp", "tp"),
            P("sp", None),
            P("sp", None),
            P(),
            P(None, "tp"),
            P(None, "tp"),
            P(None, "tp"),
            P(None, "tp"),
            P("tp"),
            P("tp"),
            P("tp", None),
            P("tp", None),
            P(),
            P("sp", "tp"),
            P("sp", "tp"),
            P(None, "tp"),
            P(None, "tp"),
            P("tp", None),
            P("tp"),
        ),
        out_specs=P("sp", "tp"),
        check_vma=False,
    )
```

```python
import jax
import jax.numpy as jnp
from jax import lax
from jax.experimental import pallas as pl
from jax.experimental.pallas import tpu as pltpu
from jax.sharding import PartitionSpec as P

D = 2048
HA = 16
DA = 64
HB = 8
DB = 128
DR = 32
KC = 3


THETA = 10000.0
EPS_RMS = 1e-06
EPS_NORM = 1e-05
ALPHA = 2.0**0.25


def passed_along(value, axis, steps):
    count = lax.axis_size(axis)
    leading, last = (max(0, -steps), min(count, count - steps))
    return lax.ppermute(value, axis, [(source, source + steps) for source in range(leading, last)])


def rotary(values, positions):
    half = values.shape[-1] // 2
    freq = THETA ** (-jnp.arange(half, dtype=jnp.float32) * 2.0 / values.shape[-1])
    angle = positions.astype(jnp.float32)[:, None] * freq[None, :]
    if values.ndim == 3:
        angle = angle[:, None, :]
    cosine = jnp.cos(angle)
    sine = jnp.sin(angle)
    first = values[..., :half]
    second = values[..., half:]
    return jnp.concatenate(
        [first * cosine - second * sine, second * cosine + first * sine], axis=-1
    )


def rms_scale(values, gain):
    wide = values.astype(jnp.float32)
    return wide * lax.rsqrt(jnp.mean(wide * wide, axis=-1, keepdims=True) + EPS_RMS) * gain


def row_norm(values, gain):
    center = jnp.mean(values, axis=1, keepdims=True)
    shifted = values - center
    spread = jnp.mean(shifted * shifted, axis=1, keepdims=True)
    return shifted * lax.rsqrt(spread + EPS_NORM) * gain


def xor_swap(value, axis, mask):
    count = lax.axis_size(axis)
    return lax.ppermute(value, axis, [(source, source ^ mask) for source in range(count)])


def natural_order(items, index):
    bit = 1
    while bit < len(items):
        flip = (index & bit) != 0
        items = [jnp.where(flip, items[k ^ bit], items[k]) for k in range(len(items))]
        bit *= 2
    return items


def peer_sum(value, axis):
    if lax.axis_size(axis) == 2:
        return value + xor_swap(value, axis, 1)
    return lax.psum(value, axis)


def peer_blocks(value, axis):
    if lax.axis_size(axis) == 2:
        return jnp.stack(natural_order([value, xor_swap(value, axis, 1)], lax.axis_index(axis)))
    return lax.all_gather(value, axis, axis=0)


GROUP = 4
VMEM_SPEC = pl.BlockSpec(memory_space=pltpu.VMEM)
SMEM_SPEC = pl.BlockSpec(memory_space=pltpu.SMEM)
PARAMS = pltpu.CompilerParams(vmem_limit_bytes=56 * 1024 * 1024)


def split_width(columns):
    main = columns // (128 * GROUP) * 128
    return main, (columns - GROUP * main) // GROUP


def cut_columns(weights, member):
    rows, columns = weights[0].shape
    main, rest = split_width(columns)
    count = len(weights)

    def body(*refs):
        index_ref = refs[0]
        sources = refs[1 : 1 + count]
        targets = refs[1 + count :]
        for k in range(GROUP):
            block = index_ref[0] ^ k
            for w in range(count):
                target = targets[w * GROUP + k]
                if main:
                    start = pl.multiple_of(block * main, 128)
                    target[:, :main] = sources[w][:, pl.ds(start, main)]
                if rest:
                    shape = (GROUP * rest, rest)
                    row = lax.broadcasted_iota(jnp.int32, shape, 0)
                    col = lax.broadcasted_iota(jnp.int32, shape, 1)
                    pick = jnp.where(row == col + block * rest, 1.0, 0.0).astype(jnp.bfloat16)
                    tail = sources[w][:, GROUP * main :]
                    target[:, main:] = jnp.dot(
                        tail, pick, preferred_element_type=jnp.float32
                    ).astype(jnp.bfloat16)

    shape = jax.ShapeDtypeStruct((rows, main + rest), jnp.bfloat16)
    out = pl.pallas_call(
        body,
        out_shape=[shape] * (count * GROUP),
        in_specs=[SMEM_SPEC] + [VMEM_SPEC] * count,
        out_specs=[VMEM_SPEC] * (count * GROUP),
        compiler_params=PARAMS,
        name="cut_columns",
    )(jnp.reshape(member, (1,)).astype(jnp.int32), *weights)
    return [out[w * GROUP : (w + 1) * GROUP] for w in range(count)]


def up_hidden(rows, order, gate_parts, val_parts, taps_gate, taps_val, tok_rows):
    parts = len(gate_parts)
    depth, block_rows, width = gate_parts[0].shape
    total_rows, features = rows.shape
    rim = KC - 1
    per_part = depth * block_rows
    aligned = block_rows % 128 == 0
    if not aligned:
        rows = rows.reshape(total_rows, -1, block_rows)[:, order].reshape(total_rows, features)

    def body(*refs):
        order_ref, rows_ref = refs[:2]
        gates = refs[2 : 2 + parts]
        vals = refs[2 + parts : 2 + 2 * parts]
        taps = refs[2 + 2 * parts : 4 + 2 * parts]
        outs = refs[4 + 2 * parts : 4 + 2 * parts + GROUP]
        sorted_ref, gate_ext, val_ext = refs[4 + 2 * parts + GROUP :]
        for i in range(parts * depth if aligned else 0):
            start = pl.multiple_of(order_ref[i] * block_rows, 128)
            sorted_ref[:, i * block_rows : (i + 1) * block_rows] = rows_ref[
                :, pl.ds(start, block_rows)
            ]
        source_ref = sorted_ref if aligned else rows_ref
        for sources, ext in ((gates, gate_ext), (vals, val_ext)):
            total = None
            for p in range(parts):
                term = jnp.dot(
                    source_ref[:, p * per_part : (p + 1) * per_part],
                    sources[p][...].reshape(per_part, width),
                    preferred_element_type=jnp.float32,
                )
                total = term if total is None else total + term
            total = total.astype(jnp.bfloat16).astype(jnp.float32)
            for k in range(GROUP):
                ext[k, 8 : 8 + tok_rows] = total[k * tok_rows : (k + 1) * tok_rows]
                first_rim = GROUP * tok_rows + k * 8
                ext[k, 0:8] = total[first_rim : first_rim + 8]
        for k in range(GROUP):
            sums = []
            for ext, tap_ref in ((gate_ext, taps[0]), (val_ext, taps[1])):
                total = None
                for tap in range(KC):
                    term = tap_ref[tap : tap + 1] * ext[k, 8 - rim + tap : 8 - rim + tap + tok_rows]
                    total = term if total is None else total + term
                sums.append(total)
            gate_c, val_c = sums
            hidden = gate_c / (1.0 + jnp.exp(-gate_c)) * val_c
            outs[k][...] = hidden.astype(jnp.bfloat16)

    return pl.pallas_call(
        body,
        out_shape=[jax.ShapeDtypeStruct((tok_rows, width), jnp.bfloat16)] * GROUP,
        in_specs=[SMEM_SPEC] + [VMEM_SPEC] * (3 + 2 * parts),
        out_specs=[VMEM_SPEC] * GROUP,
        scratch_shapes=[
            pltpu.VMEM((total_rows, features), jnp.bfloat16),
            pltpu.VMEM((GROUP, tok_rows + 8, width), jnp.float32),
            pltpu.VMEM((GROUP, tok_rows + 8, width), jnp.float32),
        ],
        compiler_params=PARAMS,
        name="up_hidden",
    )(order, rows, *gate_parts, *val_parts, taps_gate, taps_val)


def shards(
    resid,
    qa_nope,
    qb_nope,
    qa_rope,
    qb_rope,
    latent,
    key_rope,
    lat_gain,
    wa_key,
    wa_val,
    wb_key,
    wb_val,
    gain_a,
    gain_b,
    wa_out,
    wb_out,
    norm1_gain,
    ffn_gate,
    ffn_val,
    conv_gate,
    conv_val,
    ffn_down,
    norm2_gain,
):
    tok_rows = resid.shape[0]
    here = lax.axis_index("sp")
    core = lax.axis_index("tp")
    n_sp = lax.axis_size("sp")
    n_tp = lax.axis_size("tp")
    group = GROUP
    stride = n_sp // group
    member = here // stride
    place = here % stride
    positions = here * tok_rows + jnp.arange(tok_rows)
    heads_a = qa_nope.shape[1] // DA
    heads_b = qb_nope.shape[1] // DB
    main, rest = split_width(ffn_gate.shape[1])
    width = main + rest

    share = tok_rows // n_tp
    share_pos = here * tok_rows + core * share + jnp.arange(share)
    lat_part = lax.dynamic_slice_in_dim(latent, core * share, share, 0)
    key_part = lax.dynamic_slice_in_dim(key_rope, core * share, share, 0)
    packed = jnp.concatenate(
        [
            rms_scale(lat_part, lat_gain).astype(jnp.bfloat16),
            rotary(key_part.astype(jnp.float32), share_pos).astype(jnp.bfloat16),
        ],
        axis=1,
    )
    gathered = jnp.stack(
        [packed] + [xor_swap(packed, "sp", k * stride) for k in range(1, group)]
    )
    block_of = [here ^ (k * stride) for k in range(group)]
    block_of = jnp.stack(block_of)
    bit = 1
    while bit < stride:
        steps = [k * bit for k in range(min(4, stride // bit))]
        gathered = jnp.concatenate([xor_swap(gathered, "sp", k) if k else gathered for k in steps])
        block_of = jnp.concatenate([block_of ^ k for k in steps])
        bit *= 4
    gathered = peer_blocks(gathered, "tp")
    total_keys = n_sp * tok_rows
    key_pos = (
        block_of[None, :, None] * tok_rows
        + jnp.arange(n_tp)[:, None, None] * share
        + jnp.arange(share)[None, None, :]
    ).reshape(total_keys)
    gathered = gathered.reshape(total_keys, -1)
    lat_n = gathered[:, : latent.shape[1]]
    k_rot = gathered[:, latent.shape[1] :]

    blocks_gate, blocks_val = cut_columns([ffn_gate, ffn_val], member)

    def exchanged(blocks):
        return jnp.stack(
            [blocks[0]] + [xor_swap(blocks[k], "sp", k * stride) for k in range(1, group)]
        )

    z_gate = exchanged(blocks_gate)
    z_val = exchanged(blocks_val)
    resid_full = peer_blocks(resid, "tp")

    rot_a = rotary(qa_rope.astype(jnp.float32).reshape(tok_rows, heads_a, DR), positions).astype(
        jnp.bfloat16
    )
    rot_b = rotary(qb_rope.astype(jnp.float32).reshape(tok_rows, heads_b, DR), positions).astype(
        jnp.bfloat16
    )
    query_a = qa_nope.reshape(tok_rows, heads_a, DA)
    query_b = qb_nope.reshape(tok_rows, heads_b, DB)
    allowed = key_pos[None, :] <= positions[:, None]

    def project(weight, heads, size):
        result = jnp.dot(lat_n, weight, preferred_element_type=jnp.float32).astype(jnp.bfloat16)
        return result.reshape(total_keys, heads, size)

    def attend(query, q_rot, keys, vals):
        size = query.shape[2]
        scale = (size + DR) ** (-0.5)
        scores = jnp.einsum("qhd,khd->hqk", query, keys, preferred_element_type=jnp.float32)
        scores = (
            scores + jnp.einsum("qhr,kr->hqk", q_rot, k_rot, preferred_element_type=jnp.float32)
        ) * scale
        scores = jnp.where(allowed[None], scores, -1e30)
        weights = jnp.exp(scores - jnp.max(scores, axis=-1, keepdims=True))
        total = jnp.sum(weights, axis=-1)
        mixed = jnp.einsum(
            "hqk,khd->qhd", weights.astype(jnp.bfloat16), vals, preferred_element_type=jnp.float32
        )
        mixed = mixed / jnp.transpose(total)[:, :, None]
        return mixed.reshape(tok_rows, -1)

    raw_a = attend(query_a, rot_a, project(wa_key, heads_a, DA), project(wa_val, heads_a, DA))
    raw_b = attend(query_b, rot_b, project(wb_key, heads_b, DB), project(wb_val, heads_b, DB))
    z_gate, raw_a = lax.optimization_barrier((z_gate, raw_a))
    z_val, raw_b = lax.optimization_barrier((z_val, raw_b))
    if stride == 4:
        gate_x = xor_swap(z_gate, "sp", 1)
        val_y = xor_swap(z_val, "sp", 2)
        gate_y = xor_swap(z_gate, "sp", 2)
        val_x = xor_swap(z_val, "sp", 1)
    energy = jnp.sum(raw_a * raw_a, axis=1, keepdims=True) + jnp.sum(
        raw_b * raw_b, axis=1, keepdims=True
    )
    partial_value = jnp.dot(
        (raw_a * gain_a).astype(jnp.bfloat16), wa_out, preferred_element_type=jnp.float32
    ) + jnp.dot((raw_b * gain_b).astype(jnp.bfloat16), wb_out, preferred_element_type=jnp.float32)
    energy = peer_sum(energy, "tp")
    head_factor = lax.rsqrt(energy / (HA * DA + HB * DB) + EPS_RMS)
    mix = peer_sum(partial_value.astype(jnp.bfloat16), "tp").astype(jnp.float32) * head_factor
    resid_rows = jnp.concatenate([resid_full[k] for k in range(n_tp)], axis=1)
    first = row_norm(ALPHA * resid_rows.astype(jnp.float32) + mix, norm1_gain).astype(jnp.bfloat16)

    columns = resid.shape[1]
    half = lax.dynamic_slice_in_dim(first, core * columns, columns, 1)
    halves = jnp.stack(
        [half] + [xor_swap(half, "sp", k * stride) for k in range(1, group)]
    ).reshape(group * tok_rows, columns)
    rim_rows = first[tok_rows - 8 :]
    rims = []
    for k in range(group):
        pairs = [
            (s, ((s // stride) ^ k) * stride + (s % stride + 1) % stride) for s in range(n_sp)
        ]
        rims.append(lax.ppermute(rim_rows, "sp", pairs))
    by_member = natural_order(rims, member)
    edge = [jnp.zeros_like(rim_rows)] + by_member[:-1]
    by_member = [jnp.where(place == 0, edge[k], by_member[k]) for k in range(group)]
    rims = natural_order(by_member, member)
    both = peer_blocks(halves, "tp")
    group_rows = jnp.concatenate(
        [jnp.concatenate([both[k] for k in range(n_tp)], axis=1)] + rims, axis=0
    )

    if stride == 4:
        gate_parts = [z_gate, gate_x, gate_y, xor_swap(gate_x, "sp", 2)]
        val_parts = [z_val, val_x, val_y, xor_swap(val_y, "sp", 1)]
    else:
        gate_parts, val_parts = [z_gate], [z_val]
        bit = 1
        while bit < stride:
            gate_parts = gate_parts + [xor_swap(p, "sp", bit) for p in gate_parts]
            val_parts = val_parts + [xor_swap(p, "sp", bit) for p in val_parts]
            bit *= 2
    order = jnp.stack([here ^ (k * stride + r) for r in range(stride) for k in range(group)])

    def own_taps(taps):
        return jnp.concatenate(
            [
                lax.dynamic_slice_in_dim(taps, member * main, main, 1),
                lax.dynamic_slice_in_dim(taps, group * main + member * rest, rest, 1),
            ],
            axis=1,
        )

    hidden = up_hidden(
        group_rows,
        order.astype(jnp.int32),
        gate_parts,
        val_parts,
        own_taps(conv_gate),
        own_taps(conv_val),
        tok_rows,
    )

    down = None
    for k in range(group):
        part = xor_swap(hidden[k], "sp", k * stride) if k else hidden[0]
        index = member ^ k
        spans = ((0, index * main, main), (main, group * main + index * rest, rest))
        for at, row, size in spans:
            if size:
                rows = lax.dynamic_slice_in_dim(ffn_down, row, size, 0)
                term = jnp.dot(
                    part[:, at : at + size], rows, preferred_element_type=jnp.float32
                )
                down = term if down is None else down + term
    down = peer_sum(down.astype(jnp.bfloat16), "tp").astype(jnp.float32)
    pre_two = ALPHA * first.astype(jnp.float32) + down
    center = jnp.mean(pre_two, axis=1, keepdims=True)
    spread = jnp.mean((pre_two - center) * (pre_two - center), axis=1, keepdims=True)
    mine = lax.dynamic_slice_in_dim(pre_two, core * columns, columns, 1)
    return ((mine - center) * lax.rsqrt(spread + EPS_NORM) * norm2_gain).astype(jnp.bfloat16)


def solution(mesh):
    return jax.shard_map(
        shards,
        mesh=mesh,
        in_specs=(
            P("sp", "tp"),
            P("sp", "tp"),
            P("sp", "tp"),
            P("sp", "tp"),
            P("sp", "tp"),
            P("sp", None),
            P("sp", None),
            P(),
            P(None, "tp"),
            P(None, "tp"),
            P(None, "tp"),
            P(None, "tp"),
            P("tp"),
            P("tp"),
            P("tp", None),
            P("tp", None),
            P(),
            P("sp", "tp"),
            P("sp", "tp"),
            P(None, "tp"),
            P(None, "tp"),
            P("tp", None),
            P("tp"),
        ),
        out_specs=P("sp", "tp"),
        check_vma=False,
    )
```
